32 devices in a mesh: tp: 16 (over z, y, core), dp: 2 (over x).
Axes of the slice: x: 2, y: 2, z: 4, core: 2. Of those that a mesh axis runs over, the one named last changes fastest.
Arguments:
- resid: bfloat16 [64, 2048], P('dp', 'tp'), may hold values from -6 to 6
- norm_gain: float32 [2, 2048], replicated, may hold values from 0.1 to 1.9
- w_query: bfloat16 [2, 2048, 2048], P(None, 'dp', 'tp'), may hold values from -0.125 to 0.125
- w_forget: bfloat16 [2, 2048, 2048], P(None, 'dp', 'tp'), may hold values from -0.125 to 0.125
- w_value: bfloat16 [2, 2048, 16, 128], P(None, 'dp', None, 'tp'), may hold values from -0.125 to 0.125
- w_gate: bfloat16 [2, 2048, 16, 128], P(None, 'dp', None, 'tp'), may hold values from -0.125 to 0.125
- gate_floor: float32 [2, 2048], replicated, may hold values from 0 to 0.9
- states: float32 [2, 64, 16, 128, 128], P(None, 'dp', None, 'tp'), may hold values from -1 to 1
- out_gain: float32 [2, 16, 128], P(None, None, 'tp'), may hold values from 0.1 to 1.9
- w_out: bfloat16 [2, 16, 128, 2048], P(None, None, 'tp'), may hold values from -0.125 to 0.125
Outputs:
- new_resid: bfloat16 [64, 2048], P('dp', 'tp')
- new_states: float32 [2, 64, 16, 128, 128], P(None, 'dp', None, 'tp')
The draws below stay inside these ranges and needn't reach their ends.
All inputs are finite; a program needn't handle non-finite values.
Results may differ from the reference program's by a relative error of at most 0.029.
Values may be sent and summed in bfloat16 or wider, within the bound.
No kernel may reach another device: no remote copies, remote signals or barrier semaphores. Data moves between devices by JAX's collectives and lax.ppermute only.
A program may use at most 64 MiB of HBM per device.

```python
import jax
import jax.numpy as jnp
from jax import lax

D = 2048
HEADS = 16
HD = 128
BLOCKS = 2
WIDTH = 2048
BATCH = 64
N_DP = 2


def block_scale(own_key, dims, split, low, largest):
    def one(axis_at, shards_of):
        heights = jax.random.uniform(jax.random.fold_in(jax.random.fold_in(own_key, 6), axis_at), (shards_of,), jnp.float32, low / len(split), largest / len(split))
        return jnp.repeat(jnp.exp(heights), dims[axis_at] // shards_of).reshape((-1,) + (1,) * (len(dims) - axis_at - 1))

    gain = one(*split[0])
    for cut in split[1:]:
        gain = gain * one(*cut)
    return gain


def normal_values(key, extent, deviation, bound, cuts=(), kind=jnp.bfloat16):
    values = jax.random.normal(key, extent, jnp.float32) * deviation
    if len(cuts) > 0:
        values = block_scale(key, extent, cuts, -0.22, 0.18) * values
    return jnp.clip(values, min=-bound, max=bound).astype(kind)


def setup_inputs(seed: int = 0) -> dict:
    key_of = jax.random.split(jax.random.key(seed), 11)
    return {
        "resid": normal_values(key_of[0], (BATCH, D), 1.0, 6.0, ((0, 2), (1, 16))),
        "norm_gain": jnp.clip(1.0 + 0.18 * jax.random.normal(key_of[1], (BLOCKS, D), jnp.float32), 0.1, 1.9),
        "w_query": normal_values(key_of[2], (BLOCKS, D, WIDTH), D ** -0.5, 0.125, ((1, 2), (2, 16))),
        "w_forget": normal_values(key_of[3], (BLOCKS, D, WIDTH), D ** -0.5, 0.125, ((1, 2), (2, 16))),
        "w_value": normal_values(key_of[4], (BLOCKS, D, HEADS, HD), D ** -0.5, 0.125, ((1, 2), (3, 16))),
        "w_gate": normal_values(key_of[5], (BLOCKS, D, HEADS, HD), D ** -0.5, 0.125, ((1, 2), (3, 16))),
        "gate_floor": jnp.clip(jax.random.uniform(key_of[6], (BLOCKS, WIDTH), jnp.float32, 0.0, 0.9), 0.0, 0.9),
        "states": normal_values(key_of[7], (BLOCKS, BATCH, HEADS, HD, HD), 0.15, 1.0, ((1, 2), (3, 16)), jnp.float32),
        "out_gain": jnp.clip(1.0 + 0.18 * jax.random.normal(key_of[8], (BLOCKS, HEADS, HD), jnp.float32), 0.1, 1.9),
        "w_out": normal_values(key_of[9], (BLOCKS, HEADS, HD, D), WIDTH ** -0.5, 0.125, ((2, 16),)),
    }


epsilon = 1e-06

def project(scaled, weight, inv_rms):
    row_count = weight.shape[0] // N_DP
    total = jnp.zeros((scaled.shape[0], weight.shape[1]), jnp.float32)
    for part_index in range(N_DP):
        lo_row = part_index * row_count
        partial_value = jnp.dot(scaled[:, lo_row:lo_row + row_count], weight[lo_row:lo_row + row_count], preferred_element_type=jnp.float32)
        total = total + lax.optimization_barrier(partial_value.astype(jnp.bfloat16)).astype(jnp.float32)
    return (total * inv_rms).astype(jnp.bfloat16)

def reference(resid, norm_gain, w_query, w_forget, w_value, w_gate, gate_floor, states, out_gain, w_out):
    residual = resid
    batch = resid.shape[0]
    new_list = []
    for layer in range(BLOCKS):
        resid_f32 = residual.astype(jnp.float32)
        inv_rms = lax.rsqrt(lax.optimization_barrier(jnp.mean(resid_f32 * resid_f32, axis=1, keepdims=True)) + epsilon)
        scaled = (resid_f32 * norm_gain[layer]).astype(jnp.bfloat16)
        queries = project(scaled, w_query[layer], inv_rms)
        forget_pre = project(scaled, w_forget[layer], inv_rms)
        values = project(scaled, w_value[layer].reshape(D, WIDTH), inv_rms)
        gate_pre = project(scaled, w_gate[layer].reshape(D, WIDTH), inv_rms)
        floor_now = gate_floor[layer]
        keep = floor_now + (1.0 - floor_now) * jax.nn.sigmoid(forget_pre.astype(jnp.float32))
        keep = keep.reshape(batch, HEADS, HD)
        value_f32 = values.astype(jnp.float32).reshape(batch, HEADS, HD)
        state_new = keep[:, :, None, :] * states[layer] + (1.0 - keep)[:, :, None, :] * value_f32[:, :, :, None]
        query_f32 = queries.astype(jnp.float32).reshape(batch, HEADS, HD)
        readout = lax.optimization_barrier(jnp.sum(query_f32[:, :, None, :] * state_new, axis=3))
        mean_square = lax.optimization_barrier(jnp.mean(readout * readout, axis=2, keepdims=True))
        gate_f32 = gate_pre.astype(jnp.float32).reshape(batch, HEADS, HD)
        normed = (readout * lax.rsqrt(mean_square + epsilon) * out_gain[layer] * jax.nn.silu(gate_f32)).astype(jnp.bfloat16)
        branch = jnp.dot(normed.reshape(batch, WIDTH), w_out[layer].reshape(WIDTH, D), preferred_element_type=jnp.float32)
        residual = (residual.astype(jnp.float32) + branch).astype(jnp.bfloat16)
        new_list.append(state_new)
    return (residual, jnp.stack(new_list))
```

```python
import jax
import jax.numpy as jnp
from jax import lax
from jax.sharding import PartitionSpec as P

BLOCKS = 2


epsilon = 1e-06


def gather_tp(piece, tp_size):
    copies = jnp.broadcast_to(piece[None], (tp_size,) + piece.shape)
    return lax.all_to_all(copies, "tp", 0, 0, tiled=True)


def shards(
    tp_size, dp_size,
    resid, norm_gain, w_query, w_forget, w_value, w_gate, gate_floor, states, out_gain, w_out
):
    seq_local, feat_local = resid.shape
    heads, slice_cols, head_dim = states.shape[2:]
    row_count = w_query.shape[1]
    dp_here = lax.axis_index("dp")

    weights = []
    for layer in range(BLOCKS):
        keys_own = jnp.stack([w_query[layer], w_forget[layer]])
        values_own = jnp.stack([w_value[layer], w_gate[layer]])
        parts = [(keys_own, values_own)]
        for k in range(1, dp_size):
            pairs = [(i, (i - k) % dp_size) for i in range(dp_size)]
            parts.append((lax.ppermute(keys_own, "dp", pairs), lax.ppermute(values_own, "dp", pairs)))
        weights.append(parts)

    residual = resid
    new_list = []
    for layer in range(BLOCKS):
        gathered = gather_tp(residual, tp_size)
        resid_f32 = gathered.astype(jnp.float32)
        inv_rms = lax.rsqrt(jnp.mean(resid_f32 * resid_f32, axis=(0, 2)) + epsilon)[:, None]
        gain = norm_gain[layer].reshape(tp_size, 1, feat_local)
        scaled = (resid_f32 * gain).astype(jnp.bfloat16)
        scaled = scaled.transpose(1, 0, 2).reshape(seq_local, -1)
        totals = [0.0, 0.0, 0.0, 0.0]
        for k in range(dp_size):
            lo_row = ((dp_here + k) % dp_size) * row_count
            columns = lax.dynamic_slice_in_dim(scaled, lo_row, row_count, 1)
            keys_k, values_k = weights[layer][k]
            mats = (keys_k[0], keys_k[1], values_k[0].reshape(row_count, -1), values_k[1].reshape(row_count, -1))
            totals = [
                total
                + lax.optimization_barrier(
                    jnp.dot(columns, mat, preferred_element_type=jnp.float32).astype(jnp.bfloat16)
                ).astype(jnp.float32)
                for total, mat in zip(totals, mats)
            ]
        queries, forget_pre, values, gate_pre = [
            (summed * inv_rms).astype(jnp.bfloat16) for summed in totals
        ]
        pair_all = gather_tp(jnp.concatenate([queries, forget_pre], axis=1), tp_size)
        pair_all = pair_all.astype(jnp.float32)
        query_all = pair_all[:, :, : queries.shape[1]].transpose(1, 0, 2).reshape(seq_local, heads, head_dim)
        forget_all = pair_all[:, :, queries.shape[1] :].transpose(1, 0, 2).reshape(seq_local, heads, head_dim)
        floor_now = gate_floor[layer].reshape(heads, head_dim)
        keep = floor_now + (1.0 - floor_now) * jax.nn.sigmoid(forget_all)
        value_f32 = values.astype(jnp.float32).reshape(seq_local, heads, slice_cols)
        state_new = (
            keep[:, :, None, :] * states[layer]
            + (1.0 - keep)[:, :, None, :] * value_f32[:, :, :, None]
        )
        readout = jnp.sum(query_all[:, :, None, :] * state_new, axis=3)
        power_sum = gather_tp(jnp.sum(readout * readout, axis=2), tp_size).sum(axis=0)
        mean_square = power_sum[..., None] / head_dim
        gate_f32 = gate_pre.astype(jnp.float32).reshape(seq_local, heads, slice_cols)
        normed = (
            readout * lax.rsqrt(mean_square + epsilon) * out_gain[layer] * jax.nn.silu(gate_f32)
        ).astype(jnp.bfloat16)
        flattened = normed.reshape(seq_local, heads * slice_cols)
        weight_out = w_out[layer].reshape(heads * slice_cols, -1)
        branch = jnp.dot(flattened, weight_out, preferred_element_type=jnp.float32).astype(jnp.bfloat16)
        branch = branch.reshape(seq_local, tp_size, feat_local).transpose(1, 0, 2)
        terms = lax.all_to_all(branch, "tp", 0, 0, tiled=True)
        residual = (
            residual.astype(jnp.float32) + terms.astype(jnp.float32).sum(axis=0)
        ).astype(jnp.bfloat16)
        new_list.append(state_new)
    return (residual, jnp.stack(new_list))


def solution(mesh):
    tp_size, dp_size = mesh.shape["tp"], mesh.shape["dp"]

    def body(*args):
        return shards(tp_size, dp_size, *args)

    return jax.shard_map(
        body,
        mesh=mesh,
        in_specs=(
            P("dp", "tp"),
            P(),
            P(None, "dp", "tp"),
            P(None, "dp", "tp"),
            P(None, "dp", None, "tp"),
            P(None, "dp", None, "tp"),
            P(),
            P(None, "dp", None, "tp", None),
            P(None, None, "tp"),
            P(None, None, "tp", None),
        ),
        out_specs=(P("dp", "tp"), P(None, "dp", None, "tp", None)),
        check_vma=False,
    )
```
